32 devices in a mesh: grp: 2 (over y), kv: 4 (over z), tp: 4 (over x, core).
Axes of the slice: x: 2, y: 2, z: 4, core: 2. Of those that a mesh axis runs over, the one named last changes fastest.
Arguments:
- tokens: bfloat16 [4096, 2048], P(('grp', 'kv'), 'tp'), parts along dimension 0, may hold values from -5400 to 5400, as said below
- gain: bfloat16 [2048], replicated, may hold values from 0.099609375 to 1.8984375
- w_query: bfloat16 [2048, 1024], P(None, 'tp'), may hold values from -1 to 1
- w_key: bfloat16 [2048, 512], P(None, 'tp'), may hold values from -3 to 3
- w_value: bfloat16 [2048, 512], P(None, 'tp'), may hold values from -0.125 to 0.125
- w_out: bfloat16 [1024, 2048], P(None, 'tp'), may hold values from -2 to 2
- select: int32 [32, 32], P(('grp', 'kv')), parts along dimension 0, may hold values from -1 to 63, as said below
Outputs:
- mixed: bfloat16 [4096, 2048], P(('grp', 'kv'), 'tp'), parts along dimension 0
The draws below stay inside these ranges and needn't reach their ends.
There are 2 independent parts, one for each index of `grp`. The reference program is written for one: setup_inputs(seed, part) draws one part's arguments, and reference() takes and returns one part's arrays. A program takes and returns all parts, laid end to end along the dimension named above; an argument that names none is the same for every part. Nothing has to cross between parts.
Inputs may be any that keep to these rules, and one draw needn't show every extreme that they name: Entries of tokens are finite with scales that vary by row and by column. `select`: row b lists distinct key blocks that start no later than query block b ends, or -1 for an empty slot. Every query block lists each key block of its own index of kv up to its own last position. Apart from its own index, the query blocks of one index of kv together list at most 2 distinct key blocks held by any other index; every index but the first lists exactly 2 blocks of the index before it.
All inputs are finite; a program needn't handle non-finite values.
Results may differ from the reference program's by a relative error of at most 0.012.
Values may be sent and summed in bfloat16 or wider, within the bound.
No kernel may reach another device: no remote copies, remote signals or barrier semaphores. Data moves between devices by JAX's collectives and lax.ppermute only.
A program may use at most 128 MiB of HBM per device.

```python
import math
import jax
import jax.numpy as jnp
from jax import lax

D = 2048
HEADS = 8
KV_HEADS = 4
HD = 128
TOK_DEV = 512
QB = 128
KB = 32
NSEL = 32
TOKENS = 2048
NQB = 16
NKB = 64
N_KV = 4


def draw_tokens(key, part):
    base_key = jax.random.fold_in(key, 11)
    draw_keys = jax.random.split(base_key, 3)
    column = jnp.arange(D, dtype=jnp.float32)
    base_draw = jnp.clip(jax.random.normal(draw_keys[0], (TOKENS, D), jnp.float32), -6.0, 6.0)
    rise_factor = 3.0 ** (column / D)
    row_scale = jnp.exp(jax.random.uniform(draw_keys[1], (TOKENS, 1), jnp.float32, 0.0, math.log(10.0)))
    col_scale = jnp.exp(jax.random.uniform(draw_keys[2], (1, D), jnp.float32, 0.0, math.log(10.0)))
    return (base_draw * row_scale * col_scale * rise_factor[None, :]).astype(jnp.bfloat16)


def query_weight(key):
    normal_draw = jax.random.normal(jax.random.fold_in(key, 21), (D, HEADS * HD), jnp.float32)
    return jnp.clip(normal_draw, -6.0, 6.0) / math.sqrt(D)


def draw_w_query(key, part):
    return query_weight(key).astype(jnp.bfloat16)


def draw_w_key(key, part):
    own_part = jnp.clip(jax.random.normal(jax.random.fold_in(key, 22), (D, KV_HEADS * HD), jnp.float32), -6.0, 6.0) / math.sqrt(D)
    own_part = jnp.clip(own_part, -3.0, 3.0)
    return own_part.astype(jnp.bfloat16)


def draw_select(key, part):
    base_key = jax.random.fold_in(key, 31)
    query_blocks = TOK_DEV // QB
    block_ratio = QB // KB
    blocks_dev = TOK_DEV // KB
    owner_ids = jnp.arange(N_KV, dtype=jnp.int32)
    hot_owner = (jax.random.randint(jax.random.fold_in(base_key, 1), (N_KV,), 0, 4) == 0).astype(jnp.int32)
    first_pick = jax.random.randint(jax.random.fold_in(base_key, 2), (N_KV, N_KV), 0, blocks_dev)
    step_offset = jax.random.randint(jax.random.fold_in(base_key, 3), (N_KV, N_KV), 1, blocks_dev)
    second_pick = (first_pick + step_offset) % blocks_dev
    slot_ids = jnp.arange(NSEL, dtype=jnp.int32)

    def draw_row(block_id):
        device = block_id // query_blocks
        local_block = block_id % query_blocks
        own_count = block_ratio * (local_block + 1)
        pair_count = (NSEL - own_count) // 2
        noise_bits = jax.random.randint(jax.random.fold_in(jax.random.fold_in(base_key, 4), block_id), (N_KV,), 0, 1 << 12)
        forced = (owner_ids == device - 1) | (owner_ids == device - N_KV // 2) & (device >= N_KV // 2)
        scores = noise_bits + hot_owner * (1 << 13) + forced.astype(jnp.int32) * (1 << 15)
        scores = jnp.where(owner_ids < device, scores, -(1 << 16))
        scores = scores * N_KV + owner_ids
        ranking = jnp.argsort(-scores, stable=True).astype(jnp.int32)
        rank_ids = jnp.arange(N_KV, dtype=jnp.int32)
        usable = (rank_ids < pair_count) & (ranking < device)
        block_a = ranking * blocks_dev + first_pick[device, ranking]
        block_b = ranking * blocks_dev + second_pick[device, ranking]
        pair_ids = jnp.where(usable[:, None], jnp.stack([block_a, block_b], axis=1), -1).reshape(-1)
        pair_ids = jnp.concatenate([pair_ids, jnp.full((NSEL,), -1, jnp.int32)])
        own_ids = device * blocks_dev + slot_ids
        from_pairs = jnp.take(pair_ids, jnp.maximum(slot_ids - own_count, 0))
        return jnp.where(slot_ids < own_count, own_ids, from_pairs).astype(jnp.int32)
    return jax.vmap(draw_row)(jnp.arange(NQB, dtype=jnp.int32))


def steps_of(key, shape, cuts, smallest, largest):
    level = 1.0
    for position, shards_of in cuts:
        draws = jax.random.uniform(jax.random.fold_in(jax.random.fold_in(key, 6), position), (shards_of,), jnp.float32, smallest / len(cuts), largest / len(cuts))
        level = level * jnp.repeat(jnp.exp(draws), shape[position] // shards_of).reshape((-1,) + (1,) * (len(shape) - 1 - position))
    return level


def scatter_about(key, extent, width, most, shards=(), kind=jnp.bfloat16):
    entries = width * jax.random.normal(key, extent, jnp.float32)
    if shards:
        entries = entries * steps_of(key, extent, shards, -0.22, 0.18)
    return jnp.clip(entries, -most, most).astype(kind)


def setup_inputs(seed: int = 0, part: int = 0) -> dict:
    splits = jax.random.split(jax.random.key(seed), 8)
    part_splits = jax.random.split(jax.random.fold_in(splits[7], part), 8)
    return {
        "tokens": draw_tokens(jax.random.fold_in(jax.random.fold_in(splits[7], part), 71), part),
        "gain": jnp.clip(1.0 + 0.18 * jax.random.normal(splits[1], (D,), jnp.float32), 0.099609375, 1.8984375).astype(jnp.bfloat16),
        "w_query": draw_w_query(jax.random.fold_in(splits[7], 71), part),
        "w_key": draw_w_key(jax.random.fold_in(splits[7], 71), part),
        "w_value": scatter_about(splits[4], (D, KV_HEADS * HD), D ** -0.5, 0.125, ((1, 4),)),
        "w_out": scatter_about(splits[5], (HEADS * HD, D), (max(HEADS * HD // 128, 1)) ** -0.5, 2.0, ((1, 4),)),
        "select": draw_select(jax.random.fold_in(jax.random.fold_in(splits[7], part), 71), part),
    }


epsilon = 1e-06
theta = 10000.0

def rotary(values, positions):
    head_width = values.shape[-1]
    frequency = theta ** (-jnp.arange(0, head_width, 2, dtype=jnp.float32) / head_width)
    angles = positions.astype(jnp.float32)[:, None] * frequency[None, :]
    cosine = jnp.cos(angles)[:, None, :]
    sine_table = jnp.sin(angles)[:, None, :]
    front_half = values[..., :head_width // 2]
    second = values[..., head_width // 2:]
    return jnp.concatenate([front_half * cosine - second * sine_table, second * cosine + front_half * sine_table], axis=-1)

def reference(tokens, gain, w_query, w_key, w_value, w_out, select):
    tokens_f32 = tokens.astype(jnp.float32)
    mean_square = lax.optimization_barrier(jnp.mean(tokens_f32 * tokens_f32, axis=1))
    scaled = (tokens_f32 * gain.astype(jnp.float32)[None, :]).astype(jnp.bfloat16)
    inverse = lax.rsqrt(mean_square + epsilon)[:, None]
    positions = jnp.arange(TOKENS, dtype=jnp.int32)
    query_pre = jnp.dot(scaled, w_query, preferred_element_type=jnp.float32) * inverse
    key_pre = jnp.dot(scaled, w_key, preferred_element_type=jnp.float32) * inverse
    value_pre = jnp.dot(scaled, w_value, preferred_element_type=jnp.float32) * inverse
    queries = rotary(query_pre.reshape(TOKENS, HEADS, HD), positions).astype(jnp.bfloat16)
    keys_all = rotary(key_pre.reshape(TOKENS, KV_HEADS, HD), positions).astype(jnp.bfloat16)
    values_all = value_pre.astype(jnp.bfloat16).reshape(TOKENS, KV_HEADS, HD)
    group_size = HEADS // KV_HEADS
    key_blocks = keys_all.reshape(NKB, KB, KV_HEADS, HD)
    value_blocks = values_all.reshape(NKB, KB, KV_HEADS, HD)

    def one_block(block_id):
        block_ids = select[block_id]
        safe_ids = jnp.maximum(block_ids, 0)
        keys_sel = jnp.take(key_blocks, safe_ids, axis=0).reshape(NSEL * KB, KV_HEADS, HD).astype(jnp.float32)
        values_sel = jnp.take(value_blocks, safe_ids, axis=0).reshape(NSEL * KB, KV_HEADS, HD).astype(jnp.float32)
        query_rows = lax.dynamic_slice_in_dim(queries, block_id * QB, QB, 0)
        query_rows = query_rows.reshape(QB, KV_HEADS, group_size, HD).astype(jnp.float32)
        scores = jnp.einsum('qgrd,kgd->grqk', query_rows, keys_sel) * HD ** (-0.5)
        key_pos = (safe_ids[:, None] * KB + jnp.arange(KB, dtype=jnp.int32)[None, :]).reshape(-1)
        live_keys = jnp.repeat(block_ids >= 0, KB)
        q_pos = block_id * QB + jnp.arange(QB, dtype=jnp.int32)
        allowed = live_keys[None, :] & (key_pos[None, :] <= q_pos[:, None])
        scores = jnp.where(allowed[None, None], scores, -jnp.inf)
        row_max = lax.optimization_barrier(jnp.max(scores, axis=-1, keepdims=True))
        raised = jnp.exp(scores - row_max)
        weights = (raised / lax.optimization_barrier(jnp.sum(raised, axis=-1, keepdims=True))).astype(jnp.bfloat16)
        attended = jnp.einsum('grqk,kgd->qgrd', weights.astype(jnp.float32), values_sel)
        return attended.astype(jnp.bfloat16).reshape(QB, HEADS * HD)
    attended_all = lax.map(one_block, jnp.arange(NQB, dtype=jnp.int32)).reshape(TOKENS, HEADS * HD)
    return jnp.dot(attended_all, w_out, preferred_element_type=jnp.float32).astype(jnp.bfloat16)
```

```python
import functools

import jax
import jax.numpy as jnp
from jax import lax
from jax.experimental import pallas as pl
from jax.experimental.pallas import tpu as pltpu
from jax.sharding import PartitionSpec as P

HD = 128
KB = 32
CAP = 2
LANES = 128
SUBLANES = 8

epsilon = 1e-06
theta = 10000.0

f32 = jnp.float32
bf16 = jnp.bfloat16

VMEM = pltpu.VMEM
SMEM = pltpu.SMEM


def vspec():
    return pl.BlockSpec(memory_space=VMEM)


def sspec():
    return pl.BlockSpec(memory_space=SMEM)


def swap(array, axis, mask):
    size = lax.axis_size(axis)
    return lax.ppermute(array, axis, [(i, i ^ mask) for i in range(size)])


def gather_pieces(array, axis):
    size = lax.axis_size(axis)
    pieces = {0: array}
    mask = size >> 1
    while mask:
        for known in sorted(pieces):
            if not known & (2 * mask - 1):
                pieces[known | mask] = swap(pieces[known], axis, mask)
        mask >>= 1
    return [pieces[k] for k in range(size)]


def request_kernel(info_ref, select_ref, *out_refs, kv_count, blocks_dev):
    *ask_refs, bias_ref = out_refs
    me = info_ref[1]
    listed = select_ref[...]
    query_blocks = listed.shape[0]
    lane = lax.broadcasted_iota(jnp.int32, (SUBLANES, LANES), 1)
    ceiling = jnp.int32(1 << 30)
    for shift in range(1, kv_count):
        first = (me - shift) * blocks_dev
        match = (listed >= 0) & (listed >= first) & (listed < first + blocks_dev)
        low = jnp.min(jnp.where(match, listed, ceiling))
        high = jnp.max(jnp.where(match, listed, -1))
        high = jnp.where(high > low, high, -1)
        low = jnp.where(low < ceiling, low, -1)
        ask_refs[shift - 1][...] = jnp.where(lane == 0, low, jnp.where(lane == 1, high, -1))
        bits = []
        for wanted in (low, high):
            hit = jnp.where((listed == wanted) & match, 1.0, 0.0)
            bits.append(jnp.max(hit, axis=1, keepdims=True))
        lane_here = lax.broadcasted_iota(jnp.int32, (query_blocks, CAP * KB), 1)
        hit = jnp.where(lane_here < KB, bits[0], bits[1])
        bias_ref[shift - 1] = jnp.where(hit > 0.5, 0.0, -jnp.inf)


def make_requests(info, select, kv_count, blocks_dev):
    shifts = max(kv_count - 1, 1)
    outs = [jax.ShapeDtypeStruct((SUBLANES, LANES), jnp.int32)] * (kv_count - 1)
    outs.append(jax.ShapeDtypeStruct((shifts, select.shape[0], CAP * KB), f32))
    return pl.pallas_call(
        functools.partial(request_kernel, kv_count=kv_count, blocks_dev=blocks_dev),
        out_shape=outs,
        in_specs=[sspec(), vspec()],
        out_specs=[vspec()] * len(outs),
        name="requests",
    )(info, select)


def project_kernel(info_ref, *refs, pieces, heads, row0):
    token_refs = refs[:pieces]
    gain_ref, wq_ref, wk_ref, wv_ref, cos_ref, sin_ref, q_ref, k_ref, v_ref = refs[pieces:]
    me = info_ref[0]
    rows, width = token_refs[0].shape
    step = min(rows, 128)
    for r in range(0, rows, step):
        squares = jnp.zeros((step, 1), f32)
        acc_q = jnp.zeros((step, wq_ref.shape[1]), f32)
        acc_kv = jnp.zeros((step, 2 * HD), f32)
        for k in range(pieces):
            origin = jnp.bitwise_xor(me, k)
            col = pl.multiple_of(origin * width, width)
            piece = token_refs[k][r : r + step, :].astype(f32)
            squares += jnp.sum(piece * piece, axis=1, keepdims=True)
            scaled = (piece * gain_ref[origin].astype(f32)).astype(bf16)
            acc_q += jnp.dot(scaled, wq_ref[pl.ds(col, width), :], preferred_element_type=f32)
            w_kv = jnp.concatenate([wk_ref[pl.ds(col, width), :], wv_ref[pl.ds(col, width), :]], axis=1)
            acc_kv += jnp.dot(scaled, w_kv, preferred_element_type=f32)
        inverse = lax.rsqrt(squares / (width * pieces) + epsilon)
        cos = cos_ref[row0 + r : row0 + r + step, :]
        sin = sin_ref[row0 + r : row0 + r + step, :]

        def rotate(x):
            return x * cos + pltpu.roll(x, HD // 2, 1) * sin

        for h in range(heads):
            head = acc_q[:, h * HD : (h + 1) * HD] * inverse
            q_ref[r : r + step, h * HD : (h + 1) * HD] = rotate(head).astype(bf16)
        k_ref[r : r + step, :] = rotate(acc_kv[:, :HD] * inverse).astype(bf16)
        v_ref[r : r + step, :] = (acc_kv[:, HD:] * inverse).astype(bf16)


def project(info, pieces, gain, wq, wk, wv, cos, sin, row0):
    rows = pieces[0].shape[0]
    outs = [
        jax.ShapeDtypeStruct((rows, wq.shape[1]), bf16),
        jax.ShapeDtypeStruct((rows, HD), bf16),
        jax.ShapeDtypeStruct((rows, HD), bf16),
    ]
    count = len(pieces)
    return pl.pallas_call(
        functools.partial(project_kernel, pieces=count, heads=wq.shape[1] // HD, row0=row0),
        out_shape=outs,
        in_specs=[sspec()] + [vspec()] * (count + 6),
        out_specs=[vspec()] * 3,
        cost_estimate=pl.CostEstimate(
            flops=2 * rows * wq.shape[0] * 4 * HD, transcendentals=0, bytes_accessed=6 << 20
        ),
        name="project",
    )(info, *pieces, gain, wq, wk, wv, cos, sin)


def send_kernel(info_ref, *refs, count, blocks_dev):
    asked_refs = refs[:count]
    k_ref, v_ref = refs[count : count + 2]
    out_refs = refs[count + 2 :]
    first = info_ref[1] * blocks_dev
    for n in range(count):
        for slot in range(CAP):
            block = jnp.clip(asked_refs[n][0, slot] - first, 0, blocks_dev - 1)
            row = pl.multiple_of(block * KB, KB)
            out_refs[n][slot * KB : (slot + 1) * KB, :HD] = k_ref[pl.ds(row, KB), :]
            out_refs[n][slot * KB : (slot + 1) * KB, HD:] = v_ref[pl.ds(row, KB), :]


def pick_blocks(info, asked, keys, values, blocks_dev):
    count = len(asked)
    outs = [jax.ShapeDtypeStruct((CAP * KB, 2 * HD), bf16)] * count
    return pl.pallas_call(
        functools.partial(send_kernel, count=count, blocks_dev=blocks_dev),
        out_shape=outs,
        in_specs=[sspec()] * (count + 1) + [vspec()] * 2,
        out_specs=[vspec()] * count,
        name="pick_blocks",
    )(info, *asked, keys, values)


def stack_heads(q_ref, row, rows, heads):
    return jnp.concatenate(
        [q_ref[row : row + rows, h * HD : (h + 1) * HD] for h in range(heads)], axis=0
    )


NT = (((1,), (1,)), ((), ()))


def local_kernel(q_ref, k_ref, v_ref, m_ref, l_ref, o_ref, *, query_rows, heads):
    scale = HD**-0.5
    stacked = heads * query_rows
    row_at = lax.broadcasted_iota(jnp.int32, (stacked, query_rows), 0) % query_rows
    col_at = lax.broadcasted_iota(jnp.int32, (stacked, query_rows), 1)
    causal = col_at <= row_at
    for b in range(q_ref.shape[0] // query_rows):
        q = stack_heads(q_ref, b * query_rows, query_rows, heads)
        parts = []
        for c in range(b + 1):
            s = lax.dot_general(
                q, k_ref[c * query_rows : (c + 1) * query_rows, :], NT, preferred_element_type=f32
            )
            s = s * scale
            parts.append(jnp.where(causal, s, -jnp.inf) if c == b else s)
        top = parts[0]
        for s in parts[1:]:
            top = jnp.maximum(top, s)
        m = jnp.max(top, axis=1, keepdims=True)
        total = jnp.zeros((stacked, query_rows), f32)
        out = jnp.zeros((stacked, HD), f32)
        for c, s in enumerate(parts):
            p = jnp.exp(s - m)
            total += p
            out += jnp.dot(
                p.astype(bf16), v_ref[c * query_rows : (c + 1) * query_rows, :], preferred_element_type=f32
            )
        m_ref[b] = jnp.broadcast_to(m, (stacked, LANES))
        l_ref[b] = jnp.broadcast_to(jnp.sum(total, axis=1, keepdims=True), (stacked, LANES))
        o_ref[b] = out


def attend_local(queries, keys, values, query_rows):
    rows, width = queries.shape
    heads = width // HD
    shape = jax.ShapeDtypeStruct((rows // query_rows, heads * query_rows, LANES), f32)
    return pl.pallas_call(
        functools.partial(local_kernel, query_rows=query_rows, heads=heads),
        out_shape=[shape] * 3,
        in_specs=[vspec()] * 3,
        out_specs=[vspec()] * 3,
        cost_estimate=pl.CostEstimate(
            flops=4 * rows * rows * width, transcendentals=rows * rows * heads, bytes_accessed=2 << 20
        ),
        name="attend_local",
    )(queries, keys, values)


def remote_kernel(q_ref, m_ref, l_ref, o_ref, bias_ref, *refs, query_rows, heads, block0, blocks, count):
    kv_refs = refs[:count]
    out_ref = refs[count]
    scale = HD**-0.5
    for b in range(block0, block0 + blocks):
        q = stack_heads(q_ref, b * query_rows, query_rows, heads)
        m1 = m_ref[b]
        parts = []
        m = m1[:, :1]
        for n in range(count):
            s = lax.dot_general(q, kv_refs[n][:, :HD], NT, preferred_element_type=f32)
            s = s * scale + bias_ref[n, b : b + 1, :]
            parts.append(s)
            m = jnp.maximum(m, jnp.max(s, axis=1, keepdims=True))
        shrink = jnp.exp(m1[:, :1] - m)
        total = l_ref[b][:, :1] * shrink
        out = o_ref[b] * shrink
        for n in range(count):
            p = jnp.exp(parts[n] - m)
            total += jnp.sum(p, axis=1, keepdims=True)
            out += jnp.dot(p.astype(bf16), kv_refs[n][:, HD:], preferred_element_type=f32)
        out = out / total
        for h in range(heads):
            row = (b - block0) * query_rows
            out_ref[row : row + query_rows, h * HD : (h + 1) * HD] = out[
                h * query_rows : (h + 1) * query_rows, :
            ].astype(bf16)


def attend_remote(queries, m, l, o, bias, received, query_rows, block0, blocks):
    heads = queries.shape[1] // HD
    count = len(received)
    return pl.pallas_call(
        functools.partial(
            remote_kernel,
            query_rows=query_rows,
            heads=heads,
            block0=block0,
            blocks=blocks,
            count=count,
        ),
        out_shape=jax.ShapeDtypeStruct((blocks * query_rows, heads * HD), bf16),
        in_specs=[vspec()] * (5 + count),
        out_specs=vspec(),
        name="attend_remote",
    )(queries, m, l, o, bias, *received)


def output_kernel(info_ref, *refs, pieces):
    att_refs = refs[:pieces]
    w_ref = refs[pieces]
    out_ref = refs[-1]
    me = info_ref[0]
    rows, width = att_refs[0].shape
    acc = jnp.zeros(out_ref.shape, f32)
    for k in range(pieces):
        row = pl.multiple_of(jnp.bitwise_xor(me, k) * width, width)
        acc += jnp.dot(att_refs[k][...], w_ref[pl.ds(row, width), :], preferred_element_type=f32)
    out_ref[...] = acc.astype(bf16)


def project_out(info, pieces, w_out, index, total_rows, so_far):
    rows = pieces[0].shape[0]
    count = len(pieces)
    args = [info, *pieces, w_out]
    specs = [sspec()] + [vspec()] * (count + 1)
    aliases = {}
    if so_far is not None:
        aliases = {len(args): 0}
        args.append(so_far)
        specs.append(pl.BlockSpec(memory_space=pl.ANY))
    return pl.pallas_call(
        functools.partial(output_kernel, pieces=count),
        grid=(1,),
        out_shape=jax.ShapeDtypeStruct((total_rows, w_out.shape[1]), bf16),
        in_specs=specs,
        out_specs=pl.BlockSpec((rows, w_out.shape[1]), lambda i: (index, 0)),
        input_output_aliases=aliases,
        cost_estimate=pl.CostEstimate(
            flops=2 * rows * w_out.shape[0] * w_out.shape[1], transcendentals=0, bytes_accessed=2 << 20
        ),
        name="project_out",
    )(*args)


def shift_up(array, axis, shift):
    size = lax.axis_size(axis)
    return lax.ppermute(array, axis, [(i, i + shift) for i in range(size - shift)])


def shift_down(array, axis, shift):
    size = lax.axis_size(axis)
    return lax.ppermute(array, axis, [(i, i - shift) for i in range(shift, size)])


def per_device(tokens, gain, w_query, w_key, w_value, w_out, select):
    tok_rows, width = tokens.shape
    kv_count = lax.axis_size("kv")
    tp_count = lax.axis_size("tp")
    tp_index = lax.axis_index("tp")
    kv_index = lax.axis_index("kv")
    blocks_dev = tok_rows // KB
    query_blocks = select.shape[0]
    query_rows = tok_rows // query_blocks
    info = jnp.stack([tp_index, kv_index]).astype(jnp.int32)

    pieces = gather_pieces(tokens, "tp")
    *asks, bias = make_requests(info, select, kv_count, blocks_dev)
    asked = [shift_down(asks[n], "kv", n + 1) for n in range(kv_count - 1)]

    half = HD // 2
    frequency = theta ** (-jnp.arange(0, HD, 2, dtype=f32) / HD)
    positions = kv_index * tok_rows + jnp.arange(tok_rows, dtype=jnp.int32)
    angles = positions.astype(f32)[:, None] * frequency[None, :]
    cos, sin = jnp.cos(angles), jnp.sin(angles)
    cos = jnp.concatenate([cos, cos], axis=1)
    sin = jnp.concatenate([-sin, sin], axis=1)

    gain_rows = gain.reshape(tp_count, 1, width)
    queries, keys, values = project(info, pieces, gain_rows, w_query, w_key, w_value, cos, sin, 0)
    received = []
    if kv_count > 1:
        sends = pick_blocks(info, asked, keys, values, blocks_dev)
        received = [shift_up(sends[n], "kv", n + 1) for n in range(kv_count - 1)]
    m, l, o = attend_local(queries, keys, values, query_rows)
    parts = 2 if query_blocks % 2 == 0 else 1
    blocks = query_blocks // parts
    mixed = None
    for part in range(parts):
        att = attend_remote(queries, m, l, o, bias, received, query_rows, part * blocks, blocks)
        att_pieces = gather_pieces(att, "tp")
        mixed = project_out(info, att_pieces, w_out, part, tok_rows, mixed)
    return mixed


def solution(mesh):
    placed = (
        P(("grp", "kv"), "tp"),
        P(),
        P(None, "tp"),
        P(None, "tp"),
        P(None, "tp"),
        P(None, "tp"),
        P(("grp", "kv"), None),
    )
    return jax.shard_map(
        per_device, mesh=mesh, in_specs=placed, out_specs=P(("grp", "kv"), "tp"), check_vma=False
    )
```

```python
import functools

import jax
import jax.numpy as jnp
from jax import lax
from jax.experimental import pallas as pl
from jax.experimental.pallas import tpu as pltpu
from jax.sharding import PartitionSpec as P

HD = 128
KB = 32
CAP = 2
LANES = 128
SUBLANES = 8

epsilon = 1e-06
theta = 10000.0

f32 = jnp.float32
bf16 = jnp.bfloat16

VMEM = pltpu.VMEM
SMEM = pltpu.SMEM


def vspec():
    return pl.BlockSpec(memory_space=VMEM)


PARAMS = pltpu.CompilerParams(vmem_limit_bytes=16 << 20)


def sspec():
    return pl.BlockSpec(memory_space=SMEM)


def swap(array, axis, mask):
    size = lax.axis_size(axis)
    return lax.ppermute(array, axis, [(i, i ^ mask) for i in range(size)])


def gather_pieces(array, axis):
    size = lax.axis_size(axis)
    pieces = {0: array}
    mask = size >> 1
    while mask:
        for known in sorted(pieces):
            if not known & (2 * mask - 1):
                pieces[known | mask] = swap(pieces[known], axis, mask)
        mask >>= 1
    return [pieces[k] for k in range(size)]


def request_kernel(info_ref, select_ref, *out_refs, kv_count, blocks_dev):
    *ask_refs, bias_ref = out_refs
    me = info_ref[1]
    listed = select_ref[...]
    query_blocks = listed.shape[0]
    lane = lax.broadcasted_iota(jnp.int32, (SUBLANES, LANES), 1)
    ceiling = jnp.int32(1 << 30)
    for shift in range(1, kv_count):
        first = (me - shift) * blocks_dev
        match = (listed >= 0) & (listed >= first) & (listed < first + blocks_dev)
        low = jnp.min(jnp.where(match, listed, ceiling))
        high = jnp.max(jnp.where(match, listed, -1))
        high = jnp.where(high > low, high, -1)
        low = jnp.where(low < ceiling, low, -1)
        ask_refs[shift - 1][...] = jnp.where(lane == 0, low, jnp.where(lane == 1, high, -1))
        bits = []
        for wanted in (low, high):
            hit = jnp.where((listed == wanted) & match, 1.0, 0.0)
            bits.append(jnp.max(hit, axis=1, keepdims=True))
        lane_here = lax.broadcasted_iota(jnp.int32, (query_blocks, CAP * KB), 1)
        hit = jnp.where(lane_here < KB, bits[0], bits[1])
        bias_ref[shift - 1] = jnp.where(hit > 0.5, 0.0, -jnp.inf)


def make_requests(info, select, kv_count, blocks_dev):
    shifts = max(kv_count - 1, 1)
    outs = [jax.ShapeDtypeStruct((SUBLANES, LANES), jnp.int32)] * (kv_count - 1)
    outs.append(jax.ShapeDtypeStruct((shifts, select.shape[0], CAP * KB), f32))
    return pl.pallas_call(
        functools.partial(request_kernel, kv_count=kv_count, blocks_dev=blocks_dev),
        out_shape=outs,
        in_specs=[sspec(), vspec()],
        out_specs=[vspec()] * len(outs),
        compiler_params=PARAMS,
        name="requests",
    )(info, select)


def project_kernel(info_ref, *refs, pieces, heads, row0):
    token_refs = refs[:pieces]
    gain_ref, wq_ref, wk_ref, wv_ref, cos_ref, sin_ref, q_ref, k_ref, v_ref = refs[pieces:]
    me = info_ref[0]
    rows, width = token_refs[0].shape
    step = min(rows, 128)
    for r in range(0, rows, step):
        squares = jnp.zeros((step, 1), f32)
        acc_q = jnp.zeros((step, wq_ref.shape[1]), f32)
        acc_kv = jnp.zeros((step, 2 * HD), f32)
        for k in range(pieces):
            origin = jnp.bitwise_xor(me, k)
            col = pl.multiple_of(origin * width, width)
            piece = token_refs[k][r : r + step, :].astype(f32)
            squares += jnp.sum(piece * piece, axis=1, keepdims=True)
            scaled = (piece * gain_ref[origin].astype(f32)).astype(bf16)
            acc_q += jnp.dot(scaled, wq_ref[pl.ds(col, width), :], preferred_element_type=f32)
            w_kv = jnp.concatenate([wk_ref[pl.ds(col, width), :], wv_ref[pl.ds(col, width), :]], axis=1)
            acc_kv += jnp.dot(scaled, w_kv, preferred_element_type=f32)
        inverse = lax.rsqrt(squares / (width * pieces) + epsilon)
        cos = cos_ref[row0 + r : row0 + r + step, :]
        sin = sin_ref[row0 + r : row0 + r + step, :]

        def rotate(x):
            return x * cos + pltpu.roll(x, HD // 2, 1) * sin

        for h in range(heads):
            head = acc_q[:, h * HD : (h + 1) * HD] * inverse
            q_ref[r : r + step, h * HD : (h + 1) * HD] = rotate(head).astype(bf16)
        k_ref[r : r + step, :] = rotate(acc_kv[:, :HD] * inverse).astype(bf16)
        v_ref[r : r + step, :] = (acc_kv[:, HD:] * inverse).astype(bf16)


def project(info, pieces, gain, wq, wk, wv, cos, sin, row0):
    rows = pieces[0].shape[0]
    outs = [
        jax.ShapeDtypeStruct((rows, wq.shape[1]), bf16),
        jax.ShapeDtypeStruct((rows, HD), bf16),
        jax.ShapeDtypeStruct((rows, HD), bf16),
    ]
    count = len(pieces)
    return pl.pallas_call(
        functools.partial(project_kernel, pieces=count, heads=wq.shape[1] // HD, row0=row0),
        out_shape=outs,
        in_specs=[sspec()] + [vspec()] * (count + 6),
        out_specs=[vspec()] * 3,
        cost_estimate=pl.CostEstimate(
            flops=2 * rows * wq.shape[0] * 4 * HD, transcendentals=0, bytes_accessed=6 << 20
        ),
        compiler_params=PARAMS,
        name="project",
    )(info, *pieces, gain, wq, wk, wv, cos, sin)


def send_kernel(info_ref, *refs, count, blocks_dev):
    asked_refs = refs[:count]
    k_ref, v_ref = refs[count : count + 2]
    out_refs = refs[count + 2 :]
    first = info_ref[1] * blocks_dev
    for n in range(count):
        for slot in range(CAP):
            block = jnp.clip(asked_refs[n][0, slot] - first, 0, blocks_dev - 1)
            row = pl.multiple_of(block * KB, KB)
            out_refs[n][slot * KB : (slot + 1) * KB, :HD] = k_ref[pl.ds(row, KB), :]
            out_refs[n][slot * KB : (slot + 1) * KB, HD:] = v_ref[pl.ds(row, KB), :]


def pick_blocks(info, asked, keys, values, blocks_dev):
    count = len(asked)
    outs = [jax.ShapeDtypeStruct((CAP * KB, 2 * HD), bf16)] * count
    return pl.pallas_call(
        functools.partial(send_kernel, count=count, blocks_dev=blocks_dev),
        out_shape=outs,
        in_specs=[sspec()] * (count + 1) + [vspec()] * 2,
        out_specs=[vspec()] * count,
        compiler_params=PARAMS,
        name="pick_blocks",
    )(info, *asked, keys, values)


def stack_heads(q_ref, row, rows, heads):
    return jnp.concatenate(
        [q_ref[row : row + rows, h * HD : (h + 1) * HD] for h in range(heads)], axis=0
    )


NT = (((1,), (1,)), ((), ()))


def local_kernel(q_ref, k_ref, v_ref, m_ref, l_ref, o_ref, *, query_rows, heads):
    scale = HD**-0.5
    stacked = heads * query_rows
    row_at = lax.broadcasted_iota(jnp.int32, (stacked, query_rows), 0) % query_rows
    col_at = lax.broadcasted_iota(jnp.int32, (stacked, query_rows), 1)
    causal = col_at <= row_at
    for b in range(q_ref.shape[0] // query_rows):
        q = stack_heads(q_ref, b * query_rows, query_rows, heads)
        parts = []
        for c in range(b + 1):
            s = lax.dot_general(
                q, k_ref[c * query_rows : (c + 1) * query_rows, :], NT, preferred_element_type=f32
            )
            s = s * scale
            parts.append(jnp.where(causal, s, -jnp.inf) if c == b else s)
        top = parts[0]
        for s in parts[1:]:
            top = jnp.maximum(top, s)
        m = jnp.max(top, axis=1, keepdims=True)
        total = jnp.zeros((stacked, query_rows), f32)
        out = jnp.zeros((stacked, HD), f32)
        for c, s in enumerate(parts):
            p = jnp.exp(s - m)
            total += p
            out += jnp.dot(
                p.astype(bf16), v_ref[c * query_rows : (c + 1) * query_rows, :], preferred_element_type=f32
            )
        m_ref[b] = jnp.broadcast_to(m, (stacked, LANES))
        l_ref[b] = jnp.broadcast_to(jnp.sum(total, axis=1, keepdims=True), (stacked, LANES))
        o_ref[b] = out


def attend_local(queries, keys, values, query_rows):
    rows, width = queries.shape
    heads = width // HD
    shape = jax.ShapeDtypeStruct((rows // query_rows, heads * query_rows, LANES), f32)
    return pl.pallas_call(
        functools.partial(local_kernel, query_rows=query_rows, heads=heads),
        out_shape=[shape] * 3,
        in_specs=[vspec()] * 3,
        out_specs=[vspec()] * 3,
        cost_estimate=pl.CostEstimate(
            flops=4 * rows * rows * width, transcendentals=rows * rows * heads, bytes_accessed=2 << 20
        ),
        compiler_params=PARAMS,
        name="attend_local",
    )(queries, keys, values)


def remote_kernel(q_ref, m_ref, l_ref, o_ref, bias_ref, *refs, query_rows, heads, block0, blocks, count):
    kv_refs = refs[:count]
    out_ref = refs[count]
    scale = HD**-0.5
    for b in range(block0, block0 + blocks):
        q = stack_heads(q_ref, b * query_rows, query_rows, heads)
        m1 = m_ref[b]
        parts = []
        m = m1[:, :1]
        for n in range(count):
            s = lax.dot_general(q, kv_refs[n][:, :HD], NT, preferred_element_type=f32)
            s = s * scale + bias_ref[n, b : b + 1, :]
            parts.append(s)
            m = jnp.maximum(m, jnp.max(s, axis=1, keepdims=True))
        shrink = jnp.exp(m1[:, :1] - m)
        total = l_ref[b][:, :1] * shrink
        out = o_ref[b] * shrink
        for n in range(count):
            p = jnp.exp(parts[n] - m)
            total += jnp.sum(p, axis=1, keepdims=True)
            out += jnp.dot(p.astype(bf16), kv_refs[n][:, HD:], preferred_element_type=f32)
        out = out / total
        for h in range(heads):
            row = (b - block0) * query_rows
            out_ref[row : row + query_rows, h * HD : (h + 1) * HD] = out[
                h * query_rows : (h + 1) * query_rows, :
            ].astype(bf16)


def attend_remote(queries, m, l, o, bias, received, query_rows, block0, blocks):
    heads = queries.shape[1] // HD
    count = len(received)
    return pl.pallas_call(
        functools.partial(
            remote_kernel,
            query_rows=query_rows,
            heads=heads,
            block0=block0,
            blocks=blocks,
            count=count,
        ),
        out_shape=jax.ShapeDtypeStruct((blocks * query_rows, heads * HD), bf16),
        in_specs=[vspec()] * (5 + count),
        out_specs=vspec(),
        compiler_params=PARAMS,
        name="attend_remote",
    )(queries, m, l, o, bias, *received)


def output_kernel(info_ref, *refs, pieces):
    att_refs = refs[:pieces]
    w_ref = refs[pieces]
    out_ref = refs[-1]
    me = info_ref[0]
    rows, width = att_refs[0].shape
    acc = jnp.zeros(out_ref.shape, f32)
    for k in range(pieces):
        row = pl.multiple_of(jnp.bitwise_xor(me, k) * width, width)
        acc += jnp.dot(att_refs[k][...], w_ref[pl.ds(row, width), :], preferred_element_type=f32)
    out_ref[...] = acc.astype(bf16)


def project_out(info, pieces, w_out, index, total_rows, so_far):
    rows = pieces[0].shape[0]
    count = len(pieces)
    args = [info, *pieces, w_out]
    specs = [sspec()] + [vspec()] * (count + 1)
    aliases = {}
    if so_far is not None:
        aliases = {len(args): 0}
        args.append(so_far)
        specs.append(pl.BlockSpec(memory_space=pl.ANY))
    return pl.pallas_call(
        functools.partial(output_kernel, pieces=count),
        grid=(1,),
        out_shape=jax.ShapeDtypeStruct((total_rows, w_out.shape[1]), bf16),
        in_specs=specs,
        out_specs=pl.BlockSpec((rows, w_out.shape[1]), lambda i: (index, 0)),
        input_output_aliases=aliases,
        cost_estimate=pl.CostEstimate(
            flops=2 * rows * w_out.shape[0] * w_out.shape[1], transcendentals=0, bytes_accessed=2 << 20
        ),
        compiler_params=PARAMS,
        name="project_out",
    )(*args)


def shift_up(array, axis, shift):
    size = lax.axis_size(axis)
    return lax.ppermute(array, axis, [(i, i + shift) for i in range(size - shift)])


def shift_down(array, axis, shift):
    size = lax.axis_size(axis)
    return lax.ppermute(array, axis, [(i, i - shift) for i in range(shift, size)])


def per_device(tokens, gain, w_query, w_key, w_value, w_out, select):
    tok_rows, width = tokens.shape
    kv_count = lax.axis_size("kv")
    tp_count = lax.axis_size("tp")
    tp_index = lax.axis_index("tp")
    kv_index = lax.axis_index("kv")
    blocks_dev = tok_rows // KB
    query_blocks = select.shape[0]
    query_rows = tok_rows // query_blocks
    info = jnp.stack([tp_index, kv_index]).astype(jnp.int32)

    pieces = gather_pieces(tokens, "tp")
    *asks, bias = make_requests(info, select, kv_count, blocks_dev)
    asked = [shift_down(asks[n], "kv", n + 1) for n in range(kv_count - 1)]

    half = HD // 2
    frequency = theta ** (-jnp.arange(0, HD, 2, dtype=f32) / HD)
    positions = kv_index * tok_rows + jnp.arange(tok_rows, dtype=jnp.int32)
    angles = positions.astype(f32)[:, None] * frequency[None, :]
    cos, sin = jnp.cos(angles), jnp.sin(angles)
    cos = jnp.concatenate([cos, cos], axis=1)
    sin = jnp.concatenate([-sin, sin], axis=1)

    gain_rows = gain.reshape(tp_count, 1, width)
    queries, keys, values = project(info, pieces, gain_rows, w_query, w_key, w_value, cos, sin, 0)
    received = []
    if kv_count > 1:
        sends = pick_blocks(info, asked, keys, values, blocks_dev)
        received = [shift_up(sends[n], "kv", n + 1) for n in range(kv_count - 1)]
    m, l, o = attend_local(queries, keys, values, query_rows)
    parts = 2 if query_blocks % 2 == 0 else 1
    blocks = query_blocks // parts
    mixed = None
    for part in range(parts):
        att = attend_remote(queries, m, l, o, bias, received, query_rows, part * blocks, blocks)
        att_pieces = gather_pieces(att, "tp")
        mixed = project_out(info, att_pieces, w_out, part, tok_rows, mixed)
    return mixed


def solution(mesh):
    placed = (
        P(("grp", "kv"), "tp"),
        P(),
        P(None, "tp"),
        P(None, "tp"),
        P(None, "tp"),
        P(None, "tp"),
        P(("grp", "kv"), None),
    )
    return jax.shard_map(
        per_device, mesh=mesh, in_specs=placed, out_specs=P(("grp", "kv"), "tp"), check_vma=False
    )
```
